32 devices in a mesh: grp: 2 (over y), tp: 4 (over z), dp: 4 (over x, core).
Axes of the slice: x: 2, y: 2, z: 4, core: 2. Of those that a mesh axis runs over, the one named last changes fastest.
Arguments:
- tokens: bfloat16 [128, 4096], P('grp', 'dp'), parts along dimension 0, may hold values from -6 to 6
- norm_gain: float32 [2, 4096], P(None, 'dp'), may hold values from 0.1 to 1.9
- w_query: bfloat16 [2, 4096, 512], P(None, 'dp', 'tp'), may hold values from -0.09375 to 0.09375
- w_key: bfloat16 [2, 4096, 512], P(None, 'dp', 'tp'), may hold values from -0.09375 to 0.09375
- w_value: bfloat16 [2, 4096, 512], P(None, 'dp', 'tp'), may hold values from -0.09375 to 0.09375
- w_outgate: bfloat16 [2, 4096, 512], P(None, 'dp', 'tp'), may hold values from -0.09375 to 0.09375
- gate_weight: bfloat16 [2, 4, 384, 2], P(None, 'tp'), may hold values from -0.3125 to 0.3125
- forget_bias: float32 [2, 4], P(None, 'tp'), may hold values from -2 to 4
- w_mix: bfloat16 [2, 512, 4096], P(None, 'tp', 'dp'), may hold values from -0.25 to 0.25
- memory: float32 [2, 128, 4, 128, 128], P(None, ('grp', 'dp'), 'tp'), parts along dimension 1, may hold values from -3 to 3
- normalizer: float32 [2, 128, 4, 128], P(None, ('grp', 'dp'), 'tp'), parts along dimension 1, may hold values from -3 to 3
- stabilizer: float32 [2, 128, 4], P(None, ('grp', 'dp'), 'tp'), parts along dimension 1, may hold values from -4 to 4
Outputs:
- result: bfloat16 [128, 4096], P('grp', 'dp'), parts along dimension 0
- new_memory: float32 [2, 128, 4, 128, 128], P(None, ('grp', 'dp'), 'tp'), parts along dimension 1
- new_normalizer: float32 [2, 128, 4, 128], P(None, ('grp', 'dp'), 'tp'), parts along dimension 1
- new_stabilizer: float32 [2, 128, 4], P(None, ('grp', 'dp'), 'tp'), parts along dimension 1
The draws below stay inside these ranges and needn't reach their ends.
There are 2 independent parts, one for each index of `grp`. The reference program is written for one: setup_inputs(seed, part) draws one part's arguments, and reference() takes and returns one part's arrays. A program takes and returns all parts, laid end to end along the dimension named above; an argument that names none is the same for every part. Nothing has to cross between parts.
All inputs are finite; a program needn't handle non-finite values.
Results may differ from the reference program's by a relative error of at most 0.018.
Values may be sent and summed in bfloat16 or wider, within the bound.
No kernel may reach another device: no remote copies, remote signals or barrier semaphores. Data moves between devices by JAX's collectives and lax.ppermute only.
A program may use at most 64 MiB of HBM per device.

```python
import jax
import jax.numpy as jnp
from jax import lax

D = 4096
DK = 128
BLOCKS = 2
HEADS = 4
INNER = 512
SEQS = 64


def shard_levels(key, shape, cuts, least, top_value):
    factor_of, own = 1.0, jax.random.fold_in(key, 6)
    for axis_at, parts in cuts:
        steps = jnp.exp(jax.random.uniform(jax.random.fold_in(own, axis_at), (parts,), jnp.float32, least / len(cuts), top_value / len(cuts)))
        factor_of = factor_of * jnp.repeat(steps, shape[axis_at] // parts).reshape([-1 if axis == axis_at else 1 for axis in range(len(shape))])
    return factor_of


def gaussian(stream_key, dims, spread, reach, shards=(), kind=jnp.bfloat16):
    loudness = shard_levels(stream_key, dims, shards, -0.22, 0.18) if shards else 1.0
    entries = jax.random.normal(stream_key, dims, jnp.float32) * spread * loudness
    return jnp.minimum(jnp.maximum(entries, -reach), reach).astype(kind)


def setup_inputs(seed: int = 0, part: int = 0) -> dict:
    key_list = jax.random.split(jax.random.key(seed), 13)
    part_splits = jax.random.split(jax.random.fold_in(key_list[12], part), 13)
    tokens = gaussian(part_splits[0], (SEQS, D), 1.0, 6.0, ((1, 4),))
    norm_gain = jnp.clip(1.0 + 0.18 * jax.random.normal(key_list[1], (BLOCKS, D), jnp.float32), 0.1, 1.9)
    w_query = gaussian(key_list[2], (BLOCKS, D, INNER), D ** -0.5, 0.09375, ((1, 4), (2, 4)))
    w_key = gaussian(key_list[3], (BLOCKS, D, INNER), D ** -0.5, 0.09375, ((1, 4), (2, 4)))
    w_value = gaussian(key_list[4], (BLOCKS, D, INNER), D ** -0.5, 0.09375, ((1, 4), (2, 4)))
    w_outgate = gaussian(key_list[5], (BLOCKS, D, INNER), D ** -0.5, 0.09375, ((1, 4), (2, 4)))
    gate_weight = gaussian(key_list[6], (BLOCKS, HEADS, 3 * DK, 2), (3 * DK) ** -0.5, 0.3125, ((1, 4),))
    forget_bias = jnp.clip(-2.0 + 6.0 * jax.random.uniform(key_list[7], (BLOCKS, HEADS), jnp.float32) ** shard_levels(key_list[7], (BLOCKS, HEADS), ((1, 4),), -0.2, 0.2), -2.0, 4.0)
    w_mix = gaussian(key_list[8], (BLOCKS, INNER, D), INNER ** -0.5, 0.25, ((1, 4), (2, 4)))
    memory = gaussian(part_splits[9], (BLOCKS, SEQS, HEADS, DK, DK), 0.3, 3.0, ((1, 4), (2, 4)), jnp.float32)
    normalizer = gaussian(part_splits[10], (BLOCKS, SEQS, HEADS, DK), 0.3, 3.0, ((1, 4), (2, 4)), jnp.float32)
    stabilizer = gaussian(part_splits[11], (BLOCKS, SEQS, HEADS), 1.0, 4.0, ((1, 4), (2, 4)), jnp.float32)
    return dict(tokens=tokens, norm_gain=norm_gain, w_query=w_query, w_key=w_key, w_value=w_value, w_outgate=w_outgate, gate_weight=gate_weight, forget_bias=forget_bias, w_mix=w_mix, memory=memory, normalizer=normalizer, stabilizer=stabilizer)


EPS = 1e-06

def reference(tokens, norm_gain, w_query, w_key, w_value, w_outgate, gate_weight, forget_bias, w_mix, memory, normalizer, stabilizer):
    x = tokens
    mems, norms, stabs = ([], [], [])
    seqs = tokens.shape[0]
    for blk in range(BLOCKS):
        xf = x.astype(jnp.float32)
        squares = lax.optimization_barrier(jnp.sum(xf * xf, axis=-1))
        scale = lax.rsqrt(squares / D + EPS)
        scaled_in = (xf * norm_gain[blk]).astype(jnp.bfloat16)
        projs = []
        for weight in (w_query, w_key, w_value, w_outgate):
            prod = jnp.dot(scaled_in, weight[blk], preferred_element_type=jnp.float32)
            projs.append((scale[:, None] * prod).astype(jnp.bfloat16).astype(jnp.float32).reshape(seqs, HEADS, DK))
        query, key, value, outgate = projs
        joined = jnp.concatenate([query, key, value], axis=-1)
        pre = jnp.einsum('shc,hcg->shg', joined, gate_weight[blk].astype(jnp.float32), precision=lax.Precision.HIGHEST)
        log_input = pre[..., 0]
        log_forget = jax.nn.log_sigmoid(pre[..., 1] + forget_bias[blk])
        stab = stabilizer[blk]
        new_stab = jnp.maximum(log_forget + stab, log_input)
        keep = jnp.exp(log_forget + stab - new_stab)
        admit = jnp.exp(log_input - new_stab)
        scaled_key = key * DK ** (-0.5)
        new_mem = keep[..., None, None] * memory[blk] + admit[..., None, None] * scaled_key[..., :, None] * value[..., None, :]
        new_norm = keep[..., None] * normalizer[blk] + admit[..., None] * scaled_key
        numer = jnp.einsum('shd,shde->she', query, new_mem, precision=lax.Precision.HIGHEST)
        denom = jnp.maximum(jnp.abs(lax.optimization_barrier(jnp.sum(query * new_norm, axis=-1))), 1.0)
        readout = numer / denom[..., None]
        gated = (readout * jax.nn.sigmoid(outgate)).reshape(seqs, HEADS * DK).astype(jnp.bfloat16)
        mixed = jnp.dot(gated, w_mix[blk], preferred_element_type=jnp.float32)
        x = (xf + mixed).astype(jnp.bfloat16)
        mems.append(new_mem)
        norms.append(new_norm)
        stabs.append(new_stab)
    return (x, jnp.stack(mems, axis=0), jnp.stack(norms, axis=0), jnp.stack(stabs, axis=0))
```

```python
import functools

import jax
import jax.numpy as jnp
from jax import lax
from jax.experimental import pallas as pl
from jax.experimental.pallas import tpu as pltpu
from jax.sharding import PartitionSpec as P

EPS = 1e-06
LANES = 128


def is_pow2(n):
    return n & (n - 1) == 0


def dest(i, s, n):
    return i ^ s if is_pow2(n) else (i + s) % n


def origin(i, s, n):
    return i ^ s if is_pow2(n) else (i - s + n) % n


def shift(x, axis, s, n):
    return lax.ppermute(x, axis, [(i, dest(i, s, n)) for i in range(n)])


def project(xf, gain, w_refs, part_refs, buf, me, n_dp, seq_own):
    scaled_in = (xf * gain).astype(jnp.bfloat16)
    width = w_refs[0].shape[-1]
    for at, w_ref in enumerate(w_refs):
        buf[:, at * width:(at + 1) * width] = jnp.dot(
            scaled_in, w_ref[0], preferred_element_type=jnp.float32)
    squares = jnp.sum(xf * xf, axis=-1, keepdims=True)
    buf[:, len(w_refs) * width:] = jnp.broadcast_to(squares, (xf.shape[0], LANES))
    for s in range(n_dp):
        row = pl.multiple_of(dest(me, s, n_dp) * seq_own, seq_own)
        part_refs[s][...] = buf[pl.ds(row, seq_own), :]


def first_body(ids, x_ref, gain_ref, wq, wk, wv, wo, *rest, blk, n_dp, seq_own):
    part_refs, buf = rest[:n_dp], rest[n_dp]
    xf = x_ref[...].astype(jnp.float32)
    project(xf, gain_ref[blk:blk + 1, :], (wq, wk, wv, wo), part_refs, buf, ids[0], n_dp, seq_own)


def mix_rows(ids, x_ref, g_ref, own_ref, others, n_dp, n_tp):
    acc = x_ref[...].astype(jnp.float32)
    for s in range(n_tp):
        head = origin(ids[1], s, n_tp)
        rows = jnp.concatenate([g_ref[d, head] for d in range(n_dp)], axis=0)
        weight = own_ref[0] if s == 0 else others[s - 1][...]
        acc = acc + jnp.dot(rows, weight, preferred_element_type=jnp.float32)
    return acc.astype(jnp.bfloat16)


def mid_body(ids, x_ref, g_ref, own_ref, *rest, blk, n_dp, n_tp, seq_own):
    others, rest = rest[:n_tp - 1], rest[n_tp - 1:]
    gain_ref, wq, wk, wv, wo, x_out = rest[:6]
    part_refs, buf = rest[6:6 + n_dp], rest[6 + n_dp]
    x = mix_rows(ids, x_ref, g_ref, own_ref, others, n_dp, n_tp)
    x_out[...] = x
    project(x.astype(jnp.float32), gain_ref[blk:blk + 1, :], (wq, wk, wv, wo), part_refs, buf,
            ids[0], n_dp, seq_own)


def last_body(ids, x_ref, g_ref, own_ref, *rest, n_dp, n_tp):
    others, x_out = rest[:n_tp - 1], rest[n_tp - 1]
    x_out[...] = mix_rows(ids, x_ref, g_ref, own_ref, others, n_dp, n_tp)


def cell_body(bias, *refs, blk, n_dp, width, copies, aliased):
    parts, refs = refs[:n_dp], refs[n_dp:]
    gw_ref, mem_ref, norm_ref, stab_ref = refs[:4]
    refs = refs[4 + (3 if aliased else 0):]
    send_ref, mem_out, norm_out, stab_out = refs
    total = parts[0][...]
    for part in parts[1:]:
        total = total + part[...]
    dk = mem_ref.shape[-1]
    scale = lax.rsqrt(total[:, 4 * dk:4 * dk + 1] / width + EPS)
    q16, k16, v16, o16 = ((scale * total[:, a * dk:(a + 1) * dk]).astype(jnp.bfloat16) for a in range(4))
    query, key, value, outgate = (t.astype(jnp.float32) for t in (q16, k16, v16, o16))
    pre = sum(
        jnp.dot(t, gw_ref[0, 0, a * dk:(a + 1) * dk, :], preferred_element_type=jnp.float32)
        for a, t in enumerate((q16, k16, v16)))
    log_input = pre[:, 0:1]
    z = pre[:, 1:2] + bias[blk, 0]
    log_forget = jnp.minimum(z, 0.0) - jnp.log1p(jnp.exp(-jnp.abs(z)))
    carried = log_forget + stab_ref[0]
    new_stab = jnp.maximum(carried, log_input)
    keep = jnp.exp(carried - new_stab)
    admit = jnp.exp(log_input - new_stab)
    added = admit * (key * dk ** (-0.5))
    new_norm = keep * norm_ref[0, :, 0, :] + added
    denom = jnp.maximum(jnp.abs(jnp.sum(query * new_norm, axis=-1, keepdims=True)), 1.0)
    added_t = added.T
    query_t = query.T
    numer = []
    for s in range(query.shape[0]):
        new_mem = keep[s:s + 1, :] * mem_ref[0, s, 0] + added_t[:, s:s + 1] * value[s:s + 1, :]
        mem_out[0, s, 0] = new_mem
        numer.append(jnp.sum(query_t[:, s:s + 1] * new_mem, axis=0, keepdims=True))
    readout = jnp.concatenate(numer, axis=0) / denom
    gated = (readout * jax.nn.sigmoid(outgate)).astype(jnp.bfloat16)
    for at in range(copies):
        send_ref[at] = gated
    norm_out[0, :, 0, :] = new_norm
    stab_out[0] = new_stab


VMEM = pl.BlockSpec(memory_space=pltpu.VMEM)
SMEM = pl.BlockSpec(memory_space=pltpu.SMEM)
ANY = pl.BlockSpec(memory_space=pl.ANY)


def block_of(arr, blk):
    zeros = (0,) * (arr.ndim - 1)
    return pl.BlockSpec((1,) + arr.shape[1:], lambda *_: (blk,) + zeros)


def shards(tokens, norm_gain, w_query, w_key, w_value, w_outgate, gate_weight, forget_bias, w_mix,
           memory, normalizer, stabilizer, *, n_dp, n_tp):
    blocks, seq_own, heads_own, dk, _ = memory.shape
    assert heads_own == 1
    ids = jnp.stack([lax.axis_index("dp"), lax.axis_index("tp")]).astype(jnp.int32)
    weights = (w_query, w_key, w_value, w_outgate)
    rows, feats = tokens.shape
    wide = 4 * w_query.shape[-1] + LANES
    part_shapes = [jax.ShapeDtypeStruct((seq_own, wide), jnp.float32)] * n_dp
    buf = pltpu.VMEM((rows, wide), jnp.float32)
    x_shape = jax.ShapeDtypeStruct(tokens.shape, tokens.dtype)

    x = tokens
    parts = pl.pallas_call(
        functools.partial(first_body, blk=0, n_dp=n_dp, seq_own=seq_own),
        out_shape=part_shapes,
        grid=(1,),
        in_specs=[SMEM, VMEM, VMEM] + [block_of(w, 0) for w in weights],
        out_specs=[VMEM] * n_dp,
        scratch_shapes=[buf],
        name="project_first",
    )(ids, x, norm_gain, *weights)

    states = None
    gathered = None
    for blk in range(blocks):
        own_mix = w_mix[blk]
        if gathered is not None:
            own_mix, gathered = lax.optimization_barrier((own_mix, gathered))
        mixes = [shift(own_mix, "tp", s, n_tp) for s in range(1, n_tp)]
        if gathered is not None:
            out = pl.pallas_call(
                functools.partial(mid_body, blk=blk, n_dp=n_dp, n_tp=n_tp, seq_own=seq_own),
                out_shape=[x_shape] + part_shapes,
                grid=(1,),
                in_specs=[SMEM, VMEM, VMEM, block_of(w_mix, blk - 1)] + [VMEM] * (n_tp - 1)
                + [VMEM] + [block_of(w, blk) for w in weights],
                out_specs=[VMEM] * (1 + n_dp),
                scratch_shapes=[buf],
                name="mix_project",
            )(ids, x, gathered, w_mix, *last_mixes, norm_gain, *weights)
            x, parts = out[0], out[1:]
        last_mixes = mixes
        arrived = [parts[0]] + [shift(parts[s], "dp", s, n_dp) for s in range(1, n_dp)]
        copies = n_dp * n_tp
        state_in = () if states is None else states
        out = pl.pallas_call(
            functools.partial(cell_body, blk=blk, n_dp=n_dp, width=feats * n_dp, copies=copies,
                              aliased=states is not None),
            out_shape=[jax.ShapeDtypeStruct((copies, seq_own, dk), jnp.bfloat16)]
            + [jax.ShapeDtypeStruct(t.shape, t.dtype) for t in (memory, normalizer, stabilizer)],
            grid=(1,),
            in_specs=[SMEM] + [VMEM] * n_dp
            + [block_of(t, blk) for t in (gate_weight, memory, normalizer, stabilizer)]
            + [ANY] * len(state_in),
            out_specs=[VMEM] + [block_of(t, blk) for t in (memory, normalizer, stabilizer)],
            input_output_aliases={5 + n_dp + a: 1 + a for a in range(len(state_in))},
            name="cell",
        )(forget_bias, *arrived, gate_weight, memory, normalizer, stabilizer, *state_in)
        states = out[1:]
        gathered = lax.all_to_all(out[0], ("dp", "tp"), 0, 0, tiled=True)
        gathered = gathered.reshape(n_dp, n_tp, seq_own, dk)
    x = pl.pallas_call(
        functools.partial(last_body, n_dp=n_dp, n_tp=n_tp),
        out_shape=x_shape,
        grid=(1,),
        in_specs=[SMEM, VMEM, VMEM, block_of(w_mix, blocks - 1)] + [VMEM] * (n_tp - 1),
        out_specs=VMEM,
        name="mix_last",
    )(ids, x, gathered, w_mix, *last_mixes)
    return (x, *states)


def solution(mesh):
    in_specs = (
        P("grp", "dp"),
        P(None, "dp"),
        P(None, "dp", "tp"),
        P(None, "dp", "tp"),
        P(None, "dp", "tp"),
        P(None, "dp", "tp"),
        P(None, "tp", None, None),
        P(None, "tp"),
        P(None, "tp", "dp"),
        P(None, ("grp", "dp"), "tp", None, None),
        P(None, ("grp", "dp"), "tp", None),
        P(None, ("grp", "dp"), "tp"),
    )
    out_specs = (
        P("grp", "dp"),
        P(None, ("grp", "dp"), "tp", None, None),
        P(None, ("grp", "dp"), "tp", None),
        P(None, ("grp", "dp"), "tp"),
    )
    body = functools.partial(shards, n_dp=mesh.shape["dp"], n_tp=mesh.shape["tp"])
    return jax.shard_map(body, mesh=mesh, in_specs=in_specs, out_specs=out_specs, check_vma=False)
```

```python
import functools

import jax
import jax.numpy as jnp
from jax import lax
from jax.experimental import pallas as pl
from jax.experimental.pallas import tpu as pltpu
from jax.sharding import PartitionSpec as P


EPS = 1e-06
LANES = 128


def is_pow2(n):
    return n & (n - 1) == 0


def dest(i, s, n):
    return i ^ s if is_pow2(n) else (i + s) % n


def origin(i, s, n):
    return i ^ s if is_pow2(n) else (i - s + n) % n


def shift(x, axis, s, n):
    return lax.ppermute(x, axis, [(i, dest(i, s, n)) for i in range(n)])


def fetches(w_refs, blk, stage, sems):
    return [
        pltpu.make_async_copy(w_ref.at[blk], stage.at[at], sems.at[at])
        for at, w_ref in enumerate(w_refs)]


def project(xf, gain, loads, stage, part_refs, buf, n_dp, seq_own):
    scaled_in = (xf * gain).astype(jnp.bfloat16)
    width = stage.shape[-1]
    for at, load in enumerate(loads):
        load.wait()
        buf[:, at * width:(at + 1) * width] = jnp.dot(
            scaled_in, stage[at], preferred_element_type=jnp.float32)
    squares = jnp.sum(xf * xf, axis=-1, keepdims=True)
    buf[:, len(loads) * width:] = jnp.broadcast_to(squares, (xf.shape[0], LANES))
    me = lax.axis_index("dp")
    for s in range(n_dp):
        row = pl.multiple_of(dest(me, s, n_dp) * seq_own, seq_own)
        part_refs[s][...] = buf[pl.ds(row, seq_own), :]


def columns(half, width):
    return pl.ds(pl.multiple_of(half * width, LANES), width)


def first_body(x_ref, gain_ref, wq, wk, wv, wo, mix_ref, *rest, n_dp, n_grp, seq_own):
    part_refs, mix_outs, (buf, stage, x_buf, gain_buf, sems) = rest[:n_dp], rest[n_dp:-5], rest[-5:]
    loads = fetches((wq, wk, wv, wo), 0, stage, sems)
    early = [
        pltpu.make_async_copy(x_ref, x_buf, sems.at[len(loads) + len(mix_outs)]),
        pltpu.make_async_copy(gain_ref, gain_buf, sems.at[len(loads) + len(mix_outs) + 1])]
    half = mix_ref.shape[-1] // n_grp
    cols = columns(lax.axis_index("grp"), half)
    cuts = [
        pltpu.make_async_copy(mix_ref.at[blk, :, cols], out, sems.at[len(loads) + blk])
        for blk, out in enumerate(mix_outs)]
    for copy in early + loads + cuts:
        copy.start()
    for copy in early:
        copy.wait()
    xf = x_buf[...].astype(jnp.float32)
    project(xf, gain_buf[0:1, :], loads, stage, part_refs, buf, n_dp, seq_own)
    for copy in cuts:
        copy.wait()


def mix_rows(x_buf, g_ref, early, own, others, acc, n_dp, n_tp, n_grp):
    me, grp = lax.axis_index("tp"), lax.axis_index("grp")
    half = own.shape[-1] // n_grp
    rows = [
        jnp.concatenate([g_ref[d, origin(me, s, n_tp)] for d in range(n_dp)], axis=0)
        for s in range(n_tp)]
    for copy in early:
        copy.wait()
    acc[...] = x_buf[...].astype(jnp.float32) + jnp.dot(
        rows[0], own[...], preferred_element_type=jnp.float32)
    for h in range(n_grp):
        cols = columns(origin(grp, h, n_grp), half)
        acc[:, cols] += sum(
            jnp.dot(rows[s], others[(s - 1) * n_grp + h][...], preferred_element_type=jnp.float32)
            for s in range(1, n_tp))
    return acc[...].astype(jnp.bfloat16)


def mid_body(x_ref, g_ref, mix_ref, *rest, blk, n_dp, n_tp, n_grp, seq_own):
    count = (n_tp - 1) * n_grp
    others, rest = rest[:count], rest[count:]
    gain_ref, wq, wk, wv, wo, x_out = rest[:6]
    part_refs, (acc, own, buf, stage, x_buf, gain_buf, sems) = rest[6:6 + n_dp], rest[6 + n_dp:]
    loads = fetches((wq, wk, wv, wo), blk, stage, sems)
    early = [
        pltpu.make_async_copy(mix_ref.at[blk - 1], own, sems.at[len(loads)]),
        pltpu.make_async_copy(x_ref, x_buf, sems.at[len(loads) + 1]),
        pltpu.make_async_copy(gain_ref, gain_buf, sems.at[len(loads) + 2])]
    for copy in early + loads:
        copy.start()
    x = mix_rows(x_buf, g_ref, early, own, others, acc, n_dp, n_tp, n_grp)
    x_out[...] = x
    project(x.astype(jnp.float32), gain_buf[blk:blk + 1, :], loads, stage, part_refs, buf,
            n_dp, seq_own)


def last_body(x_ref, g_ref, mix_ref, *rest, blk, n_dp, n_tp, n_grp):
    others, (x_out, acc, own, x_buf, sems) = rest[:-5], rest[-5:]
    early = [
        pltpu.make_async_copy(mix_ref.at[blk], own, sems.at[0]),
        pltpu.make_async_copy(x_ref, x_buf, sems.at[1])]
    for copy in early:
        copy.start()
    x_out[...] = mix_rows(x_buf, g_ref, early, own, others, acc, n_dp, n_tp, n_grp)


def cell_body(bias, *refs, blk, n_dp, width, copies):
    parts, refs = refs[:n_dp], refs[n_dp:]
    gw_ref, mem_far, norm_ref, stab_ref, send_ref, keep_out, added_out, value_out, stab_out = refs[:9]
    mem_ref, sems = refs[9:]
    chunks = sems.shape[0]
    span = mem_ref.shape[0] // chunks
    loads = [
        pltpu.make_async_copy(
            mem_far.at[blk, pl.ds(c * span, span), 0], mem_ref.at[pl.ds(c * span, span)], sems.at[c])
        for c in range(chunks)]
    for copy in loads:
        copy.start()
    total = parts[0][...]
    for part in parts[1:]:
        total = total + part[...]
    dk = mem_ref.shape[-1]
    scale = lax.rsqrt(total[:, 4 * dk:4 * dk + 1] / width + EPS)
    q16, k16, v16, o16 = ((scale * total[:, a * dk:(a + 1) * dk]).astype(jnp.bfloat16) for a in range(4))
    query, key, value, outgate = (t.astype(jnp.float32) for t in (q16, k16, v16, o16))
    pre = sum(
        lax.dot_general(t, gw_ref[blk, 0, :, a * dk:(a + 1) * dk], (((1,), (1,)), ((), ())),
                        preferred_element_type=jnp.float32)
        for a, t in enumerate((q16, k16, v16)))
    log_input = pre[:, 0:1]
    z = pre[:, 1:2] + bias[0, blk]
    log_forget = jnp.minimum(z, 0.0) - jnp.log1p(jnp.exp(-jnp.abs(z)))
    stab = jnp.broadcast_to(stab_ref[blk], (LANES, stab_ref.shape[-1])).T
    carried = log_forget + stab[:, 0:1]
    new_stab = jnp.maximum(carried, log_input)
    keep = jnp.exp(carried - new_stab)
    admit = jnp.exp(log_input - new_stab)
    added = admit * (key * dk ** (-0.5))
    new_norm = keep * norm_ref[blk, :, 0, :] + added
    denom = jnp.maximum(jnp.abs(jnp.sum(query * new_norm, axis=-1, keepdims=True)), 1.0)
    query_t = query.T
    numer = []
    for s in range(query.shape[0]):
        if s % span == 0:
            loads[s // span].wait()
        numer.append(jnp.sum(query_t[:, s:s + 1] * mem_ref[s], axis=0, keepdims=True))
    overlap = jnp.sum(query * added, axis=-1, keepdims=True)
    readout = (keep * jnp.concatenate(numer, axis=0) + overlap * value) / denom
    gated = (readout * jax.nn.sigmoid(outgate)).astype(jnp.bfloat16)
    for at in range(copies):
        send_ref[at] = gated
    keep_out[...] = jnp.broadcast_to(keep, keep_out.shape)
    added_out[...] = added
    value_out[...] = value
    stab_out[...] = jnp.broadcast_to(new_stab, stab_out.shape)


def write_body(mem_ref, norm_ref, *refs, blocks, span):
    given, (mem_out, norm_out, stab_out) = refs[:4 * blocks], refs[4 * blocks:]
    for blk in range(blocks):
        @pl.when(pl.program_id(0) == blk)
        def _(blk=blk):
            keep_ref, added_ref, value_ref, stab_ref = given[4 * blk:4 * blk + 4]
            rows = pl.ds(pl.multiple_of(pl.program_id(1) * span, span), span)
            keep, added, value = keep_ref[rows, :], added_ref[rows, :], value_ref[rows, :]
            added_t = added.T
            for s in range(span):
                mem_out[0, s, 0] = (
                    keep[s:s + 1, :] * mem_ref[0, s, 0] + added_t[:, s:s + 1] * value[s:s + 1, :])
            norm_out[0, :, 0, :] = keep * norm_ref[0, :, 0, :] + added
            stab_out[0] = stab_ref[...].T[0:1, :]


VMEM = pl.BlockSpec(memory_space=pltpu.VMEM)
SMEM = pl.BlockSpec(memory_space=pltpu.SMEM)
ANY = pl.BlockSpec(memory_space=pl.ANY)


NEAR_BYTES = 2 ** 21


def near(x, room):
    return pltpu.with_memory_space_constraint(x, pltpu.VMEM) if room else x


class Far:
    def __init__(self, array):
        self.array = array


def kernel_call(body, ins, outs, scratch=(), far=False, scalars=()):
    room = sum(t.nbytes for t in ins if not isinstance(t, Far)) <= 2 * NEAR_BYTES
    out = pl.pallas_call(
        body,
        out_shape=[
            o.array if isinstance(o, Far) else o if isinstance(o, jax.ShapeDtypeStruct) else jax.ShapeDtypeStruct(*o) if far else pltpu.VMEM(*o)
            for o in outs],
        in_specs=[SMEM] * len(scalars) + [ANY if isinstance(t, Far) else VMEM for t in ins],
        out_specs=[ANY if isinstance(o, Far) else VMEM for o in outs],
        scratch_shapes=list(scratch),
    )(*scalars, *(t.array if isinstance(t, Far) else near(t, room or t.nbytes < NEAR_BYTES // 32) for t in ins))
    return list(out)


def shards(tokens, norm_gain, w_query, w_key, w_value, w_outgate, gate_weight, forget_bias, w_mix,
           memory, normalizer, stabilizer, *, n_dp, n_tp, n_grp):
    blocks, seq_own, heads_own, dk, _ = memory.shape
    assert heads_own == 1
    weights = [Far(w) for w in (w_query, w_key, w_value, w_outgate)]
    far_mix = Far(w_mix)
    rows, feats = tokens.shape
    wide = 4 * w_query.shape[-1] + LANES
    part_shapes = [((seq_own, wide), jnp.float32)] * n_dp
    buf = pltpu.VMEM((rows, wide), jnp.float32)
    acc = pltpu.VMEM((rows, feats), jnp.float32)
    stage = pltpu.VMEM((len(weights),) + w_query.shape[1:], w_query.dtype)
    own_mix = pltpu.VMEM(w_mix.shape[1:], w_mix.dtype)
    sems = pltpu.SemaphoreType.DMA((len(weights) + blocks + 2,))
    x_shape = (tokens.shape, tokens.dtype)
    sizes = dict(n_dp=n_dp, n_tp=n_tp, n_grp=n_grp)
    x_buf = pltpu.VMEM(*x_shape)
    gain_buf = pltpu.VMEM(norm_gain.shape, norm_gain.dtype)
    far_gain = Far(norm_gain)
    gate_t = gate_weight.swapaxes(2, 3)
    stab_t = stabilizer.swapaxes(1, 2)
    bias_t = forget_bias.T

    out = kernel_call(
        functools.partial(first_body, n_dp=n_dp, n_grp=n_grp, seq_own=seq_own),
        [Far(tokens), far_gain, *weights, far_mix],
        part_shapes + [Far(jax.ShapeDtypeStruct((w_mix.shape[1], feats // n_grp), w_mix.dtype))] * blocks,
        [buf, stage, x_buf, gain_buf, sems])
    parts, own_mixes = out[:n_dp], out[n_dp:]

    x = tokens
    given = []
    gathered = None
    for blk in range(blocks):
        if gathered is not None:
            out = kernel_call(
                functools.partial(mid_body, blk=blk, seq_own=seq_own, **sizes),
                [Far(x), gathered, far_mix, *mixes, far_gain, *weights],
                [jax.ShapeDtypeStruct(*x_shape)] + part_shapes, [acc, own_mix, buf, stage, x_buf, gain_buf, sems])
            x, parts = out[0], out[1:]
        arrived = [parts[0]] + [shift(parts[s], "dp", s, n_dp) for s in range(1, n_dp)]
        own = own_mixes[blk]
        if gathered is not None:
            own, _ = lax.optimization_barrier((own, x))
        pieces = [shift(own, "tp", s, n_tp) for s in range(1, n_tp)]
        small = ((seq_own, dk), jnp.float32)
        out = kernel_call(
            functools.partial(cell_body, blk=blk, n_dp=n_dp, width=feats * n_dp, copies=n_dp * n_tp),
            [*arrived, gate_t, Far(memory), normalizer, stab_t],
            [((n_dp * n_tp, seq_own, dk), jnp.bfloat16)] + [small] * 4,
            [pltpu.VMEM((seq_own, dk, dk), memory.dtype), pltpu.SemaphoreType.DMA((4,))],
            scalars=(bias_t,))
        given += out[1:]
        gathered = lax.all_to_all(out[0], ("dp", "tp"), 0, 0, tiled=True)
        gathered = gathered.reshape(n_dp, n_tp, seq_own, dk)
        mixes = []
        for piece in pieces:
            piece, _ = lax.optimization_barrier((piece, out[1]))
            mixes += [piece] + [shift(piece, "grp", h, n_grp) for h in range(1, n_grp)]
    span = seq_own // 2
    state_specs = [
        pl.BlockSpec((1, span, 1, dk, dk), lambda b, c: (b, c, 0, 0, 0)),
        pl.BlockSpec((1, span, 1, dk), lambda b, c: (b, c, 0, 0))]
    new_mem, new_norm, new_stab = pl.pallas_call(
        functools.partial(write_body, blocks=blocks, span=span),
        out_shape=[jax.ShapeDtypeStruct(t.shape, t.dtype) for t in (memory, normalizer, stab_t)],
        grid=(blocks, seq_own // span),
        in_specs=state_specs + [VMEM] * len(given),
        out_specs=state_specs + [pl.BlockSpec((1, 1, seq_own), lambda b, c: (b, 0, 0))],
        name="write_state",
    )(memory, normalizer, *(near(t, True) for t in given))
    (x,) = kernel_call(
        functools.partial(last_body, blk=blocks - 1, **sizes),
        [Far(x), gathered, far_mix, *mixes], [x_shape], [acc, own_mix, x_buf, sems],
        far=True)
    return x, new_mem, new_norm, new_stab.swapaxes(1, 2)


def solution(mesh):
    in_specs = (
        P("grp", "dp"),
        P(None, "dp"),
        P(None, "dp", "tp"),
        P(None, "dp", "tp"),
        P(None, "dp", "tp"),
        P(None, "dp", "tp"),
        P(None, "tp", None, None),
        P(None, "tp"),
        P(None, "tp", "dp"),
        P(None, ("grp", "dp"), "tp", None, None),
        P(None, ("grp", "dp"), "tp", None),
        P(None, ("grp", "dp"), "tp"),
    )
    out_specs = (
        P("grp", "dp"),
        P(None, ("grp", "dp"), "tp", None, None),
        P(None, ("grp", "dp"), "tp", None),
        P(None, ("grp", "dp"), "tp"),
    )
    body = functools.partial(shards, n_dp=mesh.shape["dp"], n_tp=mesh.shape["tp"],
                             n_grp=mesh.shape["grp"])
    return jax.shard_map(body, mesh=mesh, in_specs=in_specs, out_specs=out_specs, check_vma=False)
```

```python
import functools

import jax
import jax.numpy as jnp
from jax import lax
from jax.experimental import pallas as pl
from jax.experimental.pallas import tpu as pltpu
from jax.sharding import PartitionSpec as P


EPS = 1e-06
LANES = 128


def is_pow2(n):
    return n & (n - 1) == 0


def dest(i, s, n):
    return i ^ s if is_pow2(n) else (i + s) % n


def origin(i, s, n):
    return i ^ s if is_pow2(n) else (i - s + n) % n


def shift(x, axis, s, n):
    return lax.ppermute(x, axis, [(i, dest(i, s, n)) for i in range(n)])


def fetches(w_refs, blk, stage, sems):
    return [
        pltpu.make_async_copy(w_ref.at[blk], stage.at[at], sems.at[at])
        for at, w_ref in enumerate(w_refs)]


def project(xf, gain, loads, stage, part_refs, buf, n_dp, seq_own):
    scaled_in = (xf * gain).astype(jnp.bfloat16)
    width = stage.shape[-1]
    for at, load in enumerate(loads):
        load.wait()
        buf[:, at * width:(at + 1) * width] = jnp.dot(
            scaled_in, stage[at], preferred_element_type=jnp.float32)
    squares = jnp.sum(xf * xf, axis=-1, keepdims=True)
    buf[:, len(loads) * width:] = jnp.broadcast_to(squares, (xf.shape[0], LANES))
    me = lax.axis_index("dp")
    for s in range(n_dp):
        row = pl.multiple_of(dest(me, s, n_dp) * seq_own, seq_own)
        part_refs[s][...] = buf[pl.ds(row, seq_own), :]


def columns(half, width):
    return pl.ds(pl.multiple_of(half * width, LANES), width)


def first_body(x_ref, gain_ref, wq, wk, wv, wo, mix_ref, *rest, n_dp, n_grp, seq_own):
    part_refs, mix_outs, (buf, stage, x_buf, gain_buf, sems) = rest[:n_dp], rest[n_dp:-5], rest[-5:]
    loads = fetches((wq, wk, wv, wo), 0, stage, sems)
    early = [
        pltpu.make_async_copy(x_ref, x_buf, sems.at[len(loads) + len(mix_outs)]),
        pltpu.make_async_copy(gain_ref, gain_buf, sems.at[len(loads) + len(mix_outs) + 1])]
    half = mix_ref.shape[-1] // n_grp
    cols = columns(lax.axis_index("grp"), half)
    cuts = [
        pltpu.make_async_copy(mix_ref.at[blk, :, cols], out, sems.at[len(loads) + blk])
        for blk, out in enumerate(mix_outs)]
    for copy in early + loads + cuts:
        copy.start()
    for copy in early:
        copy.wait()
    xf = x_buf[...].astype(jnp.float32)
    project(xf, gain_buf[0:1, :], loads, stage, part_refs, buf, n_dp, seq_own)
    for copy in cuts:
        copy.wait()


def mix_rows(x_buf, g_ref, early, own, others, acc, n_dp, n_tp, n_grp):
    me, grp = lax.axis_index("tp"), lax.axis_index("grp")
    half = own.shape[-1] // n_grp
    rows = [
        jnp.concatenate([g_ref[d, origin(me, s, n_tp)] for d in range(n_dp)], axis=0)
        for s in range(n_tp)]
    for copy in early:
        copy.wait()
    acc[...] = x_buf[...].astype(jnp.float32) + jnp.dot(
        rows[0], own[...], preferred_element_type=jnp.float32)
    for h in range(n_grp):
        cols = columns(origin(grp, h, n_grp), half)
        acc[:, cols] += sum(
            jnp.dot(rows[s], others[(s - 1) * n_grp + h][...], preferred_element_type=jnp.float32)
            for s in range(1, n_tp))
    return acc[...].astype(jnp.bfloat16)


def mid_body(x_ref, g_ref, mix_ref, *rest, blk, n_dp, n_tp, n_grp, seq_own):
    count = (n_tp - 1) * n_grp
    others, rest = rest[:count], rest[count:]
    gain_ref, wq, wk, wv, wo, x_out = rest[:6]
    part_refs, (acc, own, buf, stage, x_buf, gain_buf, sems) = rest[6:6 + n_dp], rest[6 + n_dp:]
    loads = fetches((wq, wk, wv, wo), blk, stage, sems)
    early = [
        pltpu.make_async_copy(mix_ref.at[blk - 1], own, sems.at[len(loads)]),
        pltpu.make_async_copy(x_ref, x_buf, sems.at[len(loads) + 1]),
        pltpu.make_async_copy(gain_ref, gain_buf, sems.at[len(loads) + 2])]
    for copy in early + loads:
        copy.start()
    x = mix_rows(x_buf, g_ref, early, own, others, acc, n_dp, n_tp, n_grp)
    x_out[...] = x
    project(x.astype(jnp.float32), gain_buf[blk:blk + 1, :], loads, stage, part_refs, buf,
            n_dp, seq_own)


def last_body(x_ref, g_ref, mix_ref, *rest, blk, n_dp, n_tp, n_grp):
    others, (x_out, acc, own, x_buf, sems) = rest[:-5], rest[-5:]
    early = [
        pltpu.make_async_copy(mix_ref.at[blk], own, sems.at[0]),
        pltpu.make_async_copy(x_ref, x_buf, sems.at[1])]
    for copy in early:
        copy.start()
    x_out[...] = mix_rows(x_buf, g_ref, early, own, others, acc, n_dp, n_tp, n_grp)


def cell_body(bias, *refs, blk, n_dp, width, copies):
    parts, refs = refs[:n_dp], refs[n_dp:]
    gw_ref, mem_far, norm_ref, stab_ref, send_ref, keep_out, added_out, value_out, stab_out = refs[:9]
    mem_ref, sems = refs[9:]
    chunks = sems.shape[0]
    span = mem_ref.shape[0] // chunks
    loads = [
        pltpu.make_async_copy(
            mem_far.at[blk, pl.ds(c * span, span), 0], mem_ref.at[pl.ds(c * span, span)], sems.at[c])
        for c in range(chunks)]
    for copy in loads:
        copy.start()
    total = parts[0][...]
    for part in parts[1:]:
        total = total + part[...]
    dk = mem_ref.shape[-1]
    scale = lax.rsqrt(total[:, 4 * dk:4 * dk + 1] / width + EPS)
    q16, k16, v16, o16 = ((scale * total[:, a * dk:(a + 1) * dk]).astype(jnp.bfloat16) for a in range(4))
    query, key, value, outgate = (t.astype(jnp.float32) for t in (q16, k16, v16, o16))
    pre = sum(
        lax.dot_general(t, gw_ref[blk, 0, :, a * dk:(a + 1) * dk], (((1,), (1,)), ((), ())),
                        preferred_element_type=jnp.float32)
        for a, t in enumerate((q16, k16, v16)))
    log_input = pre[:, 0:1]
    z = pre[:, 1:2] + bias[0, blk]
    log_forget = jnp.minimum(z, 0.0) - jnp.log1p(jnp.exp(-jnp.abs(z)))
    stab = jnp.broadcast_to(stab_ref[blk], (LANES, stab_ref.shape[-1])).T
    carried = log_forget + stab[:, 0:1]
    new_stab = jnp.maximum(carried, log_input)
    keep = jnp.exp(carried - new_stab)
    admit = jnp.exp(log_input - new_stab)
    added = admit * (key * dk ** (-0.5))
    new_norm = keep * norm_ref[blk, :, 0, :] + added
    denom = jnp.maximum(jnp.abs(jnp.sum(query * new_norm, axis=-1, keepdims=True)), 1.0)
    query_t = query.T
    numer = []
    for s in range(query.shape[0]):
        if s % span == 0:
            loads[s // span].wait()
        numer.append(jnp.sum(query_t[:, s:s + 1] * mem_ref[s], axis=0, keepdims=True))
    overlap = jnp.sum(query * added, axis=-1, keepdims=True)
    readout = (keep * jnp.concatenate(numer, axis=0) + overlap * value) / denom
    gated = (readout * jax.nn.sigmoid(outgate)).astype(jnp.bfloat16)
    for at in range(copies):
        send_ref[at] = gated
    keep_out[...] = jnp.broadcast_to(keep, keep_out.shape)
    added_out[...] = added
    value_out[...] = value
    stab_out[...] = jnp.broadcast_to(new_stab, stab_out.shape)


def write_body(mem_ref, norm_ref, keep_ref, added_ref, value_ref, stab_ref, *refs, span):
    mem_out, norm_out, stab_out = refs[-3:]
    rows = pl.ds(pl.multiple_of(pl.program_id(0) * span, span), span)
    keep, added, value = keep_ref[rows, :], added_ref[rows, :], value_ref[rows, :]
    added_t = added.T
    for s in range(span):
        mem_out[0, s, 0] = (
            keep[s:s + 1, :] * mem_ref[0, s, 0] + added_t[:, s:s + 1] * value[s:s + 1, :])
    norm_out[0, :, 0, :] = keep * norm_ref[0, :, 0, :] + added
    stab_out[0] = stab_ref[...].T[0:1, :]


VMEM = pl.BlockSpec(memory_space=pltpu.VMEM)
SMEM = pl.BlockSpec(memory_space=pltpu.SMEM)
ANY = pl.BlockSpec(memory_space=pl.ANY)


NEAR_BYTES = 2 ** 21


def near(x, room):
    return pltpu.with_memory_space_constraint(x, pltpu.VMEM) if room else x


class Far:
    def __init__(self, array):
        self.array = array


def kernel_call(body, ins, outs, scratch=(), far=False, scalars=()):
    room = sum(t.nbytes for t in ins if not isinstance(t, Far)) <= 2 * NEAR_BYTES
    out = pl.pallas_call(
        body,
        out_shape=[
            o.array if isinstance(o, Far) else o if isinstance(o, jax.ShapeDtypeStruct) else jax.ShapeDtypeStruct(*o) if far else pltpu.VMEM(*o)
            for o in outs],
        in_specs=[SMEM] * len(scalars) + [ANY if isinstance(t, Far) else VMEM for t in ins],
        out_specs=[ANY if isinstance(o, Far) else VMEM for o in outs],
        scratch_shapes=list(scratch),
    )(*scalars, *(t.array if isinstance(t, Far) else near(t, room or t.nbytes < NEAR_BYTES // 32) for t in ins))
    return list(out)


def write_state(memory, normalizer, stab_t, given, states, blk):
    seq_own, dk = memory.shape[1], memory.shape[-1]
    span = seq_own // 2
    specs = [
        pl.BlockSpec((1, span, 1, dk, dk), lambda c: (blk, c, 0, 0, 0)),
        pl.BlockSpec((1, span, 1, dk), lambda c: (blk, c, 0, 0))]
    states = [] if states is None else states
    return pl.pallas_call(
        functools.partial(write_body, span=span),
        out_shape=[jax.ShapeDtypeStruct(t.shape, t.dtype) for t in (memory, normalizer, stab_t)],
        grid=(seq_own // span,),
        in_specs=specs + [VMEM] * len(given) + [ANY] * len(states),
        out_specs=specs + [pl.BlockSpec((1, 1, seq_own), lambda c: (blk, 0, 0))],
        input_output_aliases={2 + len(given) + a: a for a in range(len(states))},
        name="write_state",
    )(memory, normalizer, *(near(t, True) for t in given), *states)


def shards(tokens, norm_gain, w_query, w_key, w_value, w_outgate, gate_weight, forget_bias, w_mix,
           memory, normalizer, stabilizer, *, n_dp, n_tp, n_grp):
    blocks, seq_own, heads_own, dk, _ = memory.shape
    assert heads_own == 1
    weights = [Far(w) for w in (w_query, w_key, w_value, w_outgate)]
    far_mix = Far(w_mix)
    rows, feats = tokens.shape
    wide = 4 * w_query.shape[-1] + LANES
    part_shapes = [((seq_own, wide), jnp.float32)] * n_dp
    buf = pltpu.VMEM((rows, wide), jnp.float32)
    acc = pltpu.VMEM((rows, feats), jnp.float32)
    stage = pltpu.VMEM((len(weights),) + w_query.shape[1:], w_query.dtype)
    own_mix = pltpu.VMEM(w_mix.shape[1:], w_mix.dtype)
    sems = pltpu.SemaphoreType.DMA((len(weights) + blocks + 2,))
    x_shape = (tokens.shape, tokens.dtype)
    sizes = dict(n_dp=n_dp, n_tp=n_tp, n_grp=n_grp)
    x_buf = pltpu.VMEM(*x_shape)
    gain_buf = pltpu.VMEM(norm_gain.shape, norm_gain.dtype)
    far_gain = Far(norm_gain)
    gate_t = gate_weight.swapaxes(2, 3)
    stab_t = stabilizer.swapaxes(1, 2)
    bias_t = forget_bias.T

    out = kernel_call(
        functools.partial(first_body, n_dp=n_dp, n_grp=n_grp, seq_own=seq_own),
        [Far(tokens), far_gain, *weights, far_mix],
        part_shapes + [((w_mix.shape[1], feats // n_grp), w_mix.dtype)],
        [buf, stage, x_buf, gain_buf, sems])
    parts, own = out[:n_dp], out[n_dp]

    x = tokens
    given = []
    gathered = states = None
    for blk in range(blocks):
        if gathered is not None:
            out = kernel_call(
                functools.partial(mid_body, blk=blk, seq_own=seq_own, **sizes),
                [Far(x), gathered, far_mix, *mixes, far_gain, *weights],
                [jax.ShapeDtypeStruct(*x_shape)] + part_shapes, [acc, own_mix, buf, stage, x_buf, gain_buf, sems])
            x, parts = out[0], out[1:]
        arrived = [parts[0]] + [shift(parts[s], "dp", s, n_dp) for s in range(1, n_dp)]
        if gathered is None:
            pieces = [shift(own, "tp", s, n_tp) for s in range(1, n_tp)]
        small = ((seq_own, dk), jnp.float32)
        out = kernel_call(
            functools.partial(cell_body, blk=blk, n_dp=n_dp, width=feats * n_dp, copies=n_dp * n_tp),
            [*arrived, gate_t, Far(memory), normalizer, stab_t],
            [((n_dp * n_tp, seq_own, dk), jnp.bfloat16)] + [small] * 4,
            [pltpu.VMEM((seq_own, dk, dk), memory.dtype), pltpu.SemaphoreType.DMA((4,))],
            scalars=(bias_t,))
        given = out[1:]
        gathered = lax.all_to_all(out[0], ("dp", "tp"), 0, 0, tiled=True)
        gathered = gathered.reshape(n_dp, n_tp, seq_own, dk)
        mixes = []
        for piece in pieces:
            piece, _ = lax.optimization_barrier((piece, out[1]))
            mixes += [piece] + [shift(piece, "grp", h, n_grp) for h in range(1, n_grp)]
        if blk + 1 < blocks:
            part = lax.axis_index("grp") * (feats // n_grp)
            own = lax.dynamic_slice_in_dim(w_mix[blk + 1], part, feats // n_grp, 1)
            own, _ = lax.optimization_barrier((own, gathered))
            pieces = [shift(own, "tp", s, n_tp) for s in range(1, n_tp)]
        states = write_state(memory, normalizer, stab_t, given, states, blk)
    new_mem, new_norm, new_stab = states
    (x,) = kernel_call(
        functools.partial(last_body, blk=blocks - 1, **sizes),
        [Far(x), gathered, far_mix, *mixes], [x_shape], [acc, own_mix, x_buf, sems],
        far=True)
    return x, new_mem, new_norm, new_stab.swapaxes(1, 2)


def solution(mesh):
    in_specs = (
        P("grp", "dp"),
        P(None, "dp"),
        P(None, "dp", "tp"),
        P(None, "dp", "tp"),
        P(None, "dp", "tp"),
        P(None, "dp", "tp"),
        P(None, "tp", None, None),
        P(None, "tp"),
        P(None, "tp", "dp"),
        P(None, ("grp", "dp"), "tp", None, None),
        P(None, ("grp", "dp"), "tp", None),
        P(None, ("grp", "dp"), "tp"),
    )
    out_specs = (
        P("grp", "dp"),
        P(None, ("grp", "dp"), "tp", None, None),
        P(None, ("grp", "dp"), "tp", None),
        P(None, ("grp", "dp"), "tp"),
    )
    body = functools.partial(shards, n_dp=mesh.shape["dp"], n_tp=mesh.shape["tp"],
                             n_grp=mesh.shape["grp"])
    return jax.shard_map(body, mesh=mesh, in_specs=in_specs, out_specs=out_specs, check_vma=False)
```
